256 devices in a mesh: grp: 4 (over y, x), ep: 64 (over z, core).
Axes of the slice: x: 2, y: 2, z: 32, core: 2. Of those that a mesh axis runs over, the one named last changes fastest.
The devices are a block of a 4x8x32 slice.
Arguments:
- tokens: bfloat16 [1024, 2048], P(('grp', 'ep')), parts along dimension 0, may hold values from -6 to 6
- lengths: int32 [1024], P(('grp', 'ep')), parts along dimension 0, may hold values from 128 to 1024, as said below
- cache_key: bfloat16 [1024, 1024, 256], P(('grp', 'ep')), parts along dimension 0, may hold values from -6 to 6
- cache_value: bfloat16 [1024, 1024, 256], P(('grp', 'ep')), parts along dimension 0, may hold values from -6 to 6
- routes: int32 [1024, 2], P(('grp', 'ep')), parts along dimension 0, may hold values from 0 to 3, all different within a row
- route_logits: float32 [1024, 2], P(('grp', 'ep')), parts along dimension 0, may hold values from -6 to 6
- mix_gain: float32 [2048], replicated, may hold values from 0.1 to 1.9
- query_gain: float32 [64], replicated, may hold values from 0.1 to 1.9
- key_gain: float32 [64], replicated, may hold values from 0.1 to 1.9
- head_bias: float32 [16], replicated, may hold values from -9 to -3.5
- w_query: bfloat16 [2048, 1024], P('ep'), may hold values from -0.125 to 0.125
- w_key: bfloat16 [2048, 256], P('ep'), may hold values from -0.125 to 0.125
- w_value: bfloat16 [2048, 256], P('ep'), may hold values from -0.125 to 0.125
- w_out: bfloat16 [1024, 2048], P(None, 'ep'), may hold values from -0.1875 to 0.1875
- ffn_gain: float32 [2048], replicated, may hold values from 0.1 to 1.9
- w_gate: bfloat16 [2048, 28672], P(None, 'ep'), may hold values from -0.125 to 0.125
- w_up: bfloat16 [2048, 28672], P(None, 'ep'), may hold values from -0.125 to 0.125
- w_down: bfloat16 [28672, 2048], P('ep'), may hold values from -0.0625 to 0.0625
Outputs:
- output: bfloat16 [1024, 2048], P(('grp', 'ep')), parts along dimension 0
- new_key: bfloat16 [1024, 256], P(('grp', 'ep')), parts along dimension 0
- new_value: bfloat16 [1024, 256], P(('grp', 'ep')), parts along dimension 0
The draws below stay inside these ranges and needn't reach their ends.
There are 4 independent parts, one for each index of `grp`. The reference program is written for one: setup_inputs(seed, part) draws one part's arguments, and reference() takes and returns one part's arrays. A program takes and returns all parts, laid end to end along the dimension named above; an argument that names none is the same for every part. Nothing has to cross between parts.
Inputs may be any that keep to these rules, and one draw needn't show every extreme that they name: `lengths`: some sequence has all 1024 positions live.
All inputs are finite; a program needn't handle non-finite values.
Results may differ from the reference program's by a relative error of at most 0.0085.
Values may be sent and summed in bfloat16 or wider, within the bound.
A program may use at most 128 MiB of HBM per device.

```python
import jax
import jax.numpy as jnp
from jax import lax

D = 2048
HEADS = 16
KV_HEADS = 4
HEAD_DIM = 64
FF = 7168
EXPERTS = 4
TOP = 2
CACHE_LEN = 1024
BATCH = 256


def draw_lengths(key, part):
    spread = jax.random.randint(key, (BATCH,), CACHE_LEN // 8, CACHE_LEN + 1)
    chosen = jax.random.randint(jax.random.fold_in(key, 7), (), 0, BATCH)
    return jnp.where(jnp.arange(BATCH) == chosen, CACHE_LEN, spread).astype(jnp.int32)


def draw_head_bias(key, part):
    picker = jax.random.uniform(jax.random.fold_in(key, 1), (HEADS,), jnp.float32)
    quick = jax.random.uniform(jax.random.fold_in(key, 2), (HEADS,), jnp.float32, -4.5, -3.5)
    steady = jax.random.uniform(jax.random.fold_in(key, 3), (HEADS,), jnp.float32, -9.0, -7.5)
    portion = 0.5
    return jnp.where(picker < portion, quick, steady).astype(jnp.float32)


def steps_of(rng, dims, split, low, top_value):
    level, own = 1.0, jax.random.fold_in(rng, 6)
    for dim, parts in split:
        steps = jnp.exp(jax.random.uniform(jax.random.fold_in(own, dim), (parts,), jnp.float32, low / len(split), top_value / len(split)))
        level = level * jnp.repeat(steps, dims[dim] // parts).reshape([-1 if axis == dim else 1 for axis in range(len(dims))])
    return level


def distinct(key, rows, number_of, top, lift):
    ranking = jax.random.permutation(jax.random.fold_in(key, 1), number_of)
    favour = ranking
    for power in range(3):
        favour = favour * favour // number_of
    favour = favour * lift // number_of
    tickets = jax.random.randint(jax.random.fold_in(key, 2), (rows, number_of), 0, 4096) + favour
    fixed_rows = jax.random.permutation(jax.random.fold_in(key, 3), rows)[jnp.arange(number_of) % rows]
    tickets = jnp.where(jnp.arange(rows)[:, None] == fixed_rows[None, :], 1 << 14, tickets)
    priority = tickets * number_of + jnp.arange(number_of)
    return lax.top_k(priority.astype(jnp.int32), top)[1].astype(jnp.int32)


def normal_values(rng, dims, scale, bound, cuts=(), held_as=jnp.bfloat16):
    entries = scale * jax.random.normal(rng, dims, jnp.float32)
    if cuts:
        entries = entries * steps_of(rng, dims, cuts, -0.22, 0.18)
    return jnp.clip(entries, -bound, bound).astype(held_as)


def setup_inputs(seed: int = 0, part: int = 0) -> dict:
    arg_keys = jax.random.split(jax.random.key(seed), 19)
    part_keys = jax.random.split(jax.random.fold_in(arg_keys[18], part), 19)
    return {
        "tokens": normal_values(part_keys[0], (BATCH, D), 1.0, 6.0, ((0, 64),)),
        "lengths": draw_lengths(jax.random.fold_in(jax.random.fold_in(arg_keys[18], part), 71), part),
        "cache_key": normal_values(part_keys[2], (BATCH, CACHE_LEN, KV_HEADS * HEAD_DIM), 1.0, 6.0, ((0, 64),)),
        "cache_value": normal_values(part_keys[3], (BATCH, CACHE_LEN, KV_HEADS * HEAD_DIM), 1.0, 6.0, ((0, 64),)),
        "routes": distinct(part_keys[4], BATCH, EXPERTS, TOP, 4096),
        "route_logits": normal_values(part_keys[5], (BATCH, TOP), 1.5, 6.0, ((0, 64),), jnp.float32),
        "mix_gain": jnp.clip(1.0 + 0.18 * jax.random.normal(arg_keys[6], (D,), jnp.float32), 0.1, 1.9),
        "query_gain": jnp.clip(1.0 + 0.18 * jax.random.normal(arg_keys[7], (HEAD_DIM,), jnp.float32), 0.1, 1.9),
        "key_gain": jnp.clip(1.0 + 0.18 * jax.random.normal(arg_keys[8], (HEAD_DIM,), jnp.float32), 0.1, 1.9),
        "head_bias": draw_head_bias(jax.random.fold_in(arg_keys[18], 71), part),
        "w_query": normal_values(arg_keys[10], (D, HEADS * HEAD_DIM), D ** -0.5, 0.125, ((0, 64),)),
        "w_key": normal_values(arg_keys[11], (D, KV_HEADS * HEAD_DIM), D ** -0.5, 0.125, ((0, 64),)),
        "w_value": normal_values(arg_keys[12], (D, KV_HEADS * HEAD_DIM), D ** -0.5, 0.125, ((0, 64),)),
        "w_out": normal_values(arg_keys[13], (HEADS * HEAD_DIM, D), (HEADS * HEAD_DIM) ** -0.5, 0.1875, ((1, 64),)),
        "ffn_gain": jnp.clip(1.0 + 0.18 * jax.random.normal(arg_keys[14], (D,), jnp.float32), 0.1, 1.9),
        "w_gate": normal_values(arg_keys[15], (D, EXPERTS * FF), D ** -0.5, 0.125, ((1, 64),)),
        "w_up": normal_values(arg_keys[16], (D, EXPERTS * FF), D ** -0.5, 0.125, ((1, 64),)),
        "w_down": normal_values(arg_keys[17], (EXPERTS * FF, D), FF ** -0.5, 0.0625, ((0, 64),)),
    }


EPSILON = 1e-06

def rms_scaled(values, gain):
    return values * lax.rsqrt(lax.optimization_barrier(jnp.mean(values * values, axis=-1, keepdims=True)) + EPSILON) * gain

def route_weights(routes, route_logits):
    experts_iota = jnp.arange(EXPERTS, dtype=jnp.int32)[None, :]
    first_share = jax.nn.sigmoid(route_logits[:, 0:1] - route_logits[:, 1:2])
    second_share = jax.nn.sigmoid(route_logits[:, 1:2] - route_logits[:, 0:1])
    return jnp.where(routes[:, 0:1] == experts_iota, first_share, 0.0) + jnp.where(routes[:, 1:2] == experts_iota, second_share, 0.0)

def reference(tokens, lengths, cache_key, cache_value, routes, route_logits, mix_gain, query_gain, key_gain, head_bias, w_query, w_key, w_value, w_out, ffn_gain, w_gate, w_up, w_down):
    as_float = tokens.astype(jnp.float32)
    normed = rms_scaled(as_float, mix_gain).astype(jnp.bfloat16)
    queries = jnp.dot(normed, w_query, preferred_element_type=jnp.float32)
    fresh_key = jnp.dot(normed, w_key, preferred_element_type=jnp.float32)
    fresh_value = jnp.dot(normed, w_value, preferred_element_type=jnp.float32)
    batch_rows = tokens.shape[0]
    group_size = HEADS // KV_HEADS
    normed_query = rms_scaled(queries.reshape(batch_rows, HEADS, HEAD_DIM), query_gain).astype(jnp.bfloat16)
    normed_query = normed_query.reshape(batch_rows, KV_HEADS, group_size, HEAD_DIM)
    new_key = rms_scaled(fresh_key.reshape(batch_rows, KV_HEADS, HEAD_DIM), key_gain)
    new_key = new_key.reshape(batch_rows, KV_HEADS * HEAD_DIM).astype(jnp.bfloat16)
    new_value = fresh_value.astype(jnp.bfloat16)
    key_heads = cache_key.reshape(batch_rows, CACHE_LEN, KV_HEADS, HEAD_DIM).astype(jnp.float32)
    value_heads = cache_value.reshape(batch_rows, CACHE_LEN, KV_HEADS, HEAD_DIM).astype(jnp.float32)
    scores = jnp.einsum('bkgd,blkd->bkgl', normed_query.astype(jnp.float32), key_heads) * HEAD_DIM ** (-0.5)
    scores = scores + head_bias.reshape(KV_HEADS, group_size)[None, :, :, None]
    live_mask = jnp.arange(CACHE_LEN, dtype=jnp.int32)[None, None, None, :] < lengths.astype(jnp.int32)[:, None, None, None]
    remain = jnp.where(live_mask, jax.nn.log_sigmoid(-scores), 0.0)
    after_sum = lax.cumsum(remain, axis=3, reverse=True) - remain
    weights = jnp.where(live_mask, jnp.exp(jax.nn.log_sigmoid(scores) + after_sum), 0.0).astype(jnp.bfloat16)
    attended = jnp.einsum('bkgl,blkd->bkgd', weights.astype(jnp.float32), value_heads)
    attended = attended.reshape(batch_rows, HEADS * HEAD_DIM).astype(jnp.bfloat16)
    mixed = as_float + jnp.dot(attended, w_out, preferred_element_type=jnp.float32)
    expert_in = rms_scaled(mixed, ffn_gain).astype(jnp.bfloat16)
    gate_table = route_weights(routes, route_logits)
    expert_sum = jnp.zeros_like(mixed)
    for expert in range(EXPERTS):
        gate_value = jnp.dot(expert_in, w_gate[:, expert * FF:(expert + 1) * FF], preferred_element_type=jnp.float32)
        up_value = jnp.dot(expert_in, w_up[:, expert * FF:(expert + 1) * FF], preferred_element_type=jnp.float32)
        hidden = (jax.nn.silu(gate_value) * up_value * gate_table[:, expert:expert + 1]).astype(jnp.bfloat16)
        expert_sum = expert_sum + jnp.dot(hidden, w_down[expert * FF:(expert + 1) * FF], preferred_element_type=jnp.float32)
    return ((mixed + expert_sum).astype(jnp.bfloat16), new_key, new_value)
```

```python
import functools

import jax
import jax.numpy as jnp
from jax import lax
from jax.experimental import pallas as pl
from jax.experimental.pallas import tpu as pltpu
from jax.sharding import PartitionSpec as P

HEADS = 16
KV_HEADS = 4
GROUP = HEADS // KV_HEADS
HEAD_DIM = 64
FF = 7168
EXPERTS = 4
EP = "ep"
NEAR = 4
LANES = 128
EPSILON = 1e-06
F32 = jnp.float32
BF16 = jnp.bfloat16
MESH = pl.DeviceIdType.MESH


def rms_scaled(values, gain):
    return values * lax.rsqrt(jnp.mean(values * values, axis=-1, keepdims=True) + EPSILON) * gain


def route_weights(routes, route_logits):
    experts_iota = jnp.arange(EXPERTS, dtype=jnp.int32)[None, :]
    first_share = jax.nn.sigmoid(route_logits[:, 0:1] - route_logits[:, 1:2])
    second_share = jax.nn.sigmoid(route_logits[:, 1:2] - route_logits[:, 0:1])
    return jnp.where(routes[:, 0:1] == experts_iota, first_share, 0.0) + jnp.where(
        routes[:, 1:2] == experts_iota, second_share, 0.0
    )


def remote(src, dst, send_sem, recv_sem, device):
    return pltpu.make_async_remote_copy(
        src_ref=src,
        dst_ref=dst,
        send_sem=send_sem,
        recv_sem=recv_sem,
        device_id={EP: device},
        device_id_type=MESH,
    )


def greet(devices):
    barrier = pltpu.get_barrier_semaphore()
    for device in devices:
        pl.semaphore_signal(barrier, inc=1, device_id={EP: device}, device_id_type=MESH)
    pl.semaphore_wait(barrier, len(devices))


def place(chips):
    me = lax.axis_index(EP)
    z, core = lax.div(me, 2), lax.rem(me, 2)

    def at(chip, c):
        return lax.rem(chip + 2 * chips, chips) * 2 + c

    return z, core, at


def ring_kernel(chips, x_ref, wa_ref, wb_ref, qkv_ref, wb_out, a_buf, b_buf, s_send, s_recv, p_send, p_recv, o_sem):
    z, core, at = place(chips)
    right, left, partner = at(z + 1, core), at(z - 1, core), at(z, 1 - core)
    rows = wa_ref.shape[0]
    half = chips // 2
    limits = (half, half - 1)
    bufs = (a_buf, b_buf)
    greet((left, right, partner))
    loads = [pltpu.make_async_copy(w, buf.at[z, core], o_sem.at[i]) for i, (w, buf) in enumerate(((wa_ref, a_buf), (wb_ref, b_buf)))]
    for load in loads:
        load.start()

    def chip_of(flow, step):
        return lax.rem((z - step if flow == 0 else z + step) + chips, chips)

    def hop(flow, step, kind):
        block = bufs[kind].at[chip_of(flow, step - 1), core]
        return remote(block, block, s_send.at[flow, step - 1, kind], s_recv.at[flow, step - 1, kind], right if flow == 0 else left)

    def landing(flow, step, kind):
        block = bufs[kind].at[chip_of(flow, step), core]
        return remote(block, block, s_send.at[flow, step - 1, kind], s_recv.at[flow, step - 1, kind], right if flow == 0 else left)

    def hand(flow, step, kind):
        block = bufs[kind].at[chip_of(flow, step), core]
        return remote(block, block, p_send.at[flow, step, kind], p_recv.at[flow, step, kind], partner)

    def handed(flow, step, kind):
        block = bufs[kind].at[chip_of(flow, step), 1 - core]
        return remote(block, block, p_send.at[flow, step, kind], p_recv.at[flow, step, kind], partner)

    def add(chip):
        block = jnp.concatenate([a_buf[chip, 0], a_buf[chip, 1]], axis=0)
        qkv_ref[...] += jnp.dot(x_ref[chip], block, preferred_element_type=F32)

    for kind in (0, 1):
        loads[kind].wait()
        for flow in (0, 1):
            hop(flow, 1, kind).start()
        hand(0, 0, kind).start()
    qkv_ref[...] = jnp.zeros_like(qkv_ref)

    def passing(step, flows, onward):
        for kind in (0, 1):
            for flow in flows:
                landing(flow, step, kind).wait_recv()
                if flow in onward:
                    hop(flow, step + 1, kind).start()
                hand(flow, step, kind).start()

    def taking(step, flows):
        for flow in flows:
            for kind in (0, 1):
                handed(flow, step, kind).wait_recv()
            add(chip_of(flow, step))

    passing(1, (0, 1), (0, 1))
    taking(0, (0,))

    def body(step, carry):
        passing(step, (0, 1), (0, 1))
        taking(step - 1, (0, 1))
        return carry

    lax.fori_loop(2, half - 1, body, 0)
    passing(half - 1, (0, 1), (0,))
    taking(half - 2, (0, 1))
    passing(half, (0,), ())
    taking(half - 1, (0, 1))
    taking(half, (0,))

    out = pltpu.make_async_copy(b_buf, wb_out, o_sem.at[2])
    out.start()

    def drained(step, carry):
        for kind in (0, 1):
            for flow in (0, 1):
                hop(flow, step, kind).wait_send()
                hand(flow, step, kind).wait_send()
        return carry

    for kind in (0, 1):
        hand(0, 0, kind).wait_send()
        hop(0, half, kind).wait_send()
        hand(0, half, kind).wait_send()
    lax.fori_loop(1, half, drained, 0)
    out.wait()


def ring(x_blocks, wa, wb, chips):
    rows, wide = wa.shape
    narrow = wb.shape[1]
    half = chips // 2
    any_space = pl.BlockSpec(memory_space=pl.ANY)
    in_vmem = pl.BlockSpec(memory_space=pltpu.VMEM)
    return pl.pallas_call(
        functools.partial(ring_kernel, chips),
        out_shape=(
            jax.ShapeDtypeStruct((x_blocks.shape[1], wide), F32),
            jax.ShapeDtypeStruct((chips, 2, rows, narrow), BF16),
        ),
        in_specs=[in_vmem, any_space, any_space],
        out_specs=(in_vmem, any_space),
        scratch_shapes=[
            pltpu.VMEM((chips, 2, rows, wide), BF16),
            pltpu.VMEM((chips, 2, rows, narrow), BF16),
            pltpu.SemaphoreType.DMA((2, half, 2)),
            pltpu.SemaphoreType.DMA((2, half, 2)),
            pltpu.SemaphoreType.DMA((2, half + 1, 2)),
            pltpu.SemaphoreType.DMA((2, half + 1, 2)),
            pltpu.SemaphoreType.DMA((3,)),
        ],
        compiler_params=pltpu.CompilerParams(collective_id=0, has_side_effects=True),
        name="weights_ring",
    )(x_blocks, wa, wb)


def near_steps(core):
    return (2 - 4 * core, 1 + 0 * core, -1 + 0 * core)


def rows_kernel(chips, x_ref, out_ref, split, pair, s_pair, s_far, r_far, s_near, r_near, s_hand, r_hand):
    z, core, at = place(chips)
    far_count = chips // NEAR
    a, b = lax.div(z, NEAR), lax.rem(z, NEAR)
    half = x_ref.shape[1] // 2
    partner = at(z, 1 - core)
    greet((partner, at(z + NEAR, core), at(z - NEAR, core), at(z + 1, core), at(z - 1, core), at(z + 2, core), at(z - 2, core)))
    split[0] = x_ref[:, :half]
    split[1] = x_ref[:, half:]
    swap = remote(split.at[1 - core], pair.at[core], s_pair.at[0], s_pair.at[1], partner)
    swap.start()
    pair[core] = split[core]
    remote(split.at[core], pair.at[1 - core], s_pair.at[0], s_pair.at[1], partner).wait_recv()
    out_ref[core, b, a] = jnp.concatenate([pair[0], pair[1]], axis=0).astype(BF16)

    limits = (far_count // 2, far_count // 2 - 1)

    def row_of(flow, step, home):
        return lax.rem((home - step if flow == 0 else home + step) + far_count, far_count)

    def far(flow, step):
        block = out_ref.at[core, b, row_of(flow, step - 1, a)]
        return remote(block, block, s_far.at[flow, step - 1], r_far.at[flow, step - 1], at(z + NEAR, core) if flow == 0 else at(z - NEAR, core))

    def far_landing(flow, step):
        block = out_ref.at[core, b, row_of(flow, step, a)]
        return remote(block, block, s_far.at[flow, step - 1], r_far.at[flow, step - 1], partner)

    steps = near_steps(core)
    slots = [(0, 0)] + [(f, s) for s in range(1, limits[0] + 1) for f in (0, 1) if s <= limits[f]]

    def beside(i, k):
        flow, step = slots[k]
        block = out_ref.at[core, b, row_of(flow, step, a)]
        return remote(block, block, s_near.at[i, k], r_near.at[i, k], at(z + steps[i], core))

    def beside_landing(i, k):
        flow, step = slots[k]
        source = lax.rem(z - steps[i] + 2 * chips, chips)
        block = out_ref.at[core, lax.rem(source, NEAR), row_of(flow, step, lax.div(source, NEAR))]
        return remote(block, block, s_near.at[i, k], r_near.at[i, k], partner)

    def hand(i):
        kind = b if i == 3 else lax.rem(z - steps[i] + 2 * chips, NEAR)
        block = out_ref.at[core, kind]
        return remote(block, block, s_hand.at[i], r_hand.at[i], partner)

    def handed(i):
        other = near_steps(1 - core)
        kind = b if i == 3 else lax.rem(z - other[i] + 2 * chips, NEAR)
        block = out_ref.at[1 - core, kind]
        return remote(block, block, s_hand.at[i], r_hand.at[i], partner)

    for k, (flow, step) in enumerate(slots):
        if k == 0:
            far(0, 1).start()
            far(1, 1).start()
        else:
            far_landing(flow, step).wait_recv()
            if step < limits[flow]:
                far(flow, step + 1).start()
        for i in range(3):
            beside(i, k).start()
    hand(3).start()
    for i in range(3):
        for k in range(len(slots)):
            beside_landing(i, k).wait_recv()
        hand(i).start()
    for i in range(4):
        handed(i).wait_recv()
    swap.wait_send()
    for k, (flow, step) in enumerate(slots):
        if k:
            far(flow, step).wait_send()
        for i in range(3):
            beside(i, k).wait_send()
    for i in range(4):
        hand(i).wait_send()


def all_rows(x, chips, number):
    rows, width = x.shape
    half = width // 2
    far_count = chips // NEAR
    in_vmem = pl.BlockSpec(memory_space=pltpu.VMEM)
    return pl.pallas_call(
        functools.partial(rows_kernel, chips),
        out_shape=jax.ShapeDtypeStruct((2, NEAR, far_count, 2 * rows, half), BF16),
        in_specs=[in_vmem],
        out_specs=in_vmem,
        scratch_shapes=[
            pltpu.VMEM((2, rows, half), F32),
            pltpu.VMEM((2, rows, half), F32),
            pltpu.SemaphoreType.DMA((2,)),
            pltpu.SemaphoreType.DMA((2, far_count // 2)),
            pltpu.SemaphoreType.DMA((2, far_count // 2)),
            pltpu.SemaphoreType.DMA((3, far_count)),
            pltpu.SemaphoreType.DMA((3, far_count)),
            pltpu.SemaphoreType.DMA((4,)),
            pltpu.SemaphoreType.DMA((4,)),
        ],
        compiler_params=pltpu.CompilerParams(collective_id=number, has_side_effects=True),
        name="all_rows",
    )(x)


def sums_kernel(chips, p_ref, out_ref, s0, r0, s1, r1, s2, r2, acc, mine, q_send, q_recv, n_send, n_recv, f_send, f_recv, w_sem):
    z, core, at = place(chips)
    far_count = chips // NEAR
    a, b = lax.div(z, NEAR), lax.rem(z, NEAR)
    half = p_ref.shape[3] // 2
    partner = at(z, 1 - core)
    greet((partner, at(z + NEAR, core), at(z - NEAR, core), at(z + 1, core), at(z - 1, core), at(z + 2, core), at(z - 2, core)))
    own_columns = pl.ds(pl.multiple_of(core * half, LANES), half)
    other_columns = pl.ds(pl.multiple_of((1 - core) * half, LANES), half)
    steps = near_steps(core)
    others = near_steps(1 - core)

    def kind_of(move):
        return lax.rem(z + move + chips, NEAR)

    def give(i):
        kind = b if i == 3 else kind_of(others[i])
        return remote(s0.at[kind], r0.at[kind], q_send.at[i], q_recv.at[i], partner)

    def given(i):
        kind = b if i == 3 else kind_of(steps[i])
        return remote(s0.at[kind], r0.at[kind], q_send.at[i], q_recv.at[i], partner)

    def beside(i):
        return remote(s1.at[i], r1.at[i], n_send.at[i], n_recv.at[i], at(z + steps[i], core))

    for i in range(4):
        kind = b if i == 3 else kind_of(others[i])
        s0[kind] = p_ref[kind, :, :, other_columns].astype(BF16)
        give(i).start()
    for i in range(3):
        kind = kind_of(steps[i])
        given(i).wait_recv()
        s1[i] = (p_ref[kind, :, :, own_columns] + r0[kind].astype(F32)).astype(BF16)
        beside(i).start()
    given(3).wait_recv()
    acc[...] = p_ref[b, :, :, own_columns] + r0[b].astype(F32)
    for i in range(3):
        beside(i).wait_recv()
        acc[...] += r1[i].astype(F32)

    limits = (far_count // 2, far_count // 2 - 1)

    def far(flow, step):
        return remote(
            s2.at[flow, step - 1],
            r2.at[flow, step - 1],
            f_send.at[flow, step - 1],
            f_recv.at[flow, step - 1],
            at(z + NEAR, core) if flow == 0 else at(z - NEAR, core),
        )

    for step in range(1, limits[0] + 1):
        for flow in (0, 1):
            if step > limits[flow]:
                continue
            ahead = limits[flow] + 1 - step
            row = lax.rem((a + ahead if flow == 0 else a - ahead) + far_count, far_count)
            value = acc[row]
            if step > 1:
                far(flow, step - 1).wait_recv()
                value = value + r2[flow, step - 2].astype(F32)
            s2[flow, step - 1] = value.astype(BF16)
            far(flow, step).start()
    total = acc[a]
    for flow in (1, 0):
        far(flow, limits[flow]).wait_recv()
        total = total + r2[flow, limits[flow] - 1].astype(F32)
    mine[...] = total
    swap = remote(mine, out_ref.at[core], w_sem.at[0], w_sem.at[1], partner)
    swap.start()
    out_ref[core] = total
    remote(mine, out_ref.at[1 - core], w_sem.at[0], w_sem.at[1], partner).wait_recv()
    swap.wait_send()
    for i in range(4):
        give(i).wait_send()
    for i in range(3):
        beside(i).wait_send()
    for flow in (0, 1):
        for step in range(1, limits[flow] + 1):
            far(flow, step).wait_send()


def owner_sums(partial, chips, number):
    kinds, far_count, rows, width = partial.shape
    half = width // 2
    in_vmem = pl.BlockSpec(memory_space=pltpu.VMEM)
    return pl.pallas_call(
        functools.partial(sums_kernel, chips),
        out_shape=jax.ShapeDtypeStruct((2, rows, half), F32),
        in_specs=[in_vmem],
        out_specs=in_vmem,
        scratch_shapes=[
            pltpu.VMEM((NEAR, far_count, rows, half), BF16),
            pltpu.VMEM((NEAR, far_count, rows, half), BF16),
            pltpu.VMEM((3, far_count, rows, half), BF16),
            pltpu.VMEM((3, far_count, rows, half), BF16),
            pltpu.VMEM((2, far_count // 2, rows, half), BF16),
            pltpu.VMEM((2, far_count // 2, rows, half), BF16),
            pltpu.VMEM((far_count, rows, half), F32),
            pltpu.VMEM((rows, half), F32),
            pltpu.SemaphoreType.DMA((4,)),
            pltpu.SemaphoreType.DMA((4,)),
            pltpu.SemaphoreType.DMA((3,)),
            pltpu.SemaphoreType.DMA((3,)),
            pltpu.SemaphoreType.DMA((2, far_count // 2)),
            pltpu.SemaphoreType.DMA((2, far_count // 2)),
            pltpu.SemaphoreType.DMA((2,)),
        ],
        compiler_params=pltpu.CompilerParams(collective_id=number, has_side_effects=True),
        name="owner_sums",
    )(partial)


def stick_kernel(lengths_ref, q_ref, bias_ref, k_ref, v_ref, o_ref):
    length = lengths_ref[pl.program_id(0)]
    cache_len = k_ref.shape[1]
    chunks = cache_len // LANES
    scores = lax.dot_general(q_ref[0], k_ref[0], (((1,), (1,)), ((), ())), preferred_element_type=F32)
    scores = scores * HEAD_DIM ** (-0.5) + bias_ref[...]
    live = lax.broadcasted_iota(jnp.int32, scores.shape, 1) < length
    soft = jnp.maximum(scores, 0.0) + jnp.log1p(jnp.exp(-jnp.abs(scores)))
    remain = jnp.where(live, -soft, 0.0)
    tall = jnp.concatenate([remain[:, i * LANES : (i + 1) * LANES] for i in range(chunks)], axis=0)
    below = lax.broadcasted_iota(jnp.int32, (LANES, LANES), 0) > lax.broadcasted_iota(jnp.int32, (LANES, LANES), 1)
    ones = below.astype(F32).astype(BF16)
    after = jnp.zeros_like(tall)
    rest = tall
    for _ in range(3):
        part = rest.astype(BF16)
        after = after + jnp.dot(part, ones, preferred_element_type=F32)
        rest = rest - part.astype(F32)
    totals = after[:, 0:1] + tall[:, 0:1]
    later = jnp.zeros((HEADS, 1), F32)
    pieces = [None] * chunks
    for i in reversed(range(chunks)):
        pieces[i] = after[i * HEADS : (i + 1) * HEADS] + later
        later = later + totals[i * HEADS : (i + 1) * HEADS]
    after_sum = jnp.concatenate(pieces, axis=1)
    weights = jnp.where(live, jnp.exp(scores - soft + after_sum), 0.0).astype(BF16)
    mixed = jnp.dot(weights, v_ref[0], preferred_element_type=F32)
    row_kind = lax.rem(lax.broadcasted_iota(jnp.int32, mixed.shape, 0), KV_HEADS)
    own = row_kind == lax.div(lax.broadcasted_iota(jnp.int32, mixed.shape, 1), HEAD_DIM)
    mixed = jnp.where(own, mixed, 0.0)
    for i in range(GROUP):
        o_ref[0, i : i + 1, :] = jnp.sum(mixed[i * KV_HEADS : (i + 1) * KV_HEADS], axis=0, keepdims=True)


def stick_attend(queries, lengths, cache_key, cache_value, query_gain, head_bias):
    rows = queries.shape[0]
    cache_len, width = cache_key.shape[1:]
    normed = rms_scaled(queries.reshape(rows, HEADS, HEAD_DIM), query_gain).astype(BF16)
    by_member = normed.reshape(rows, KV_HEADS, GROUP, HEAD_DIM).transpose(0, 2, 1, 3)
    eye = jnp.eye(KV_HEADS, dtype=BF16)
    spread = by_member[:, :, :, None, :] * eye[None, None, :, :, None]
    spread = spread.reshape(rows, HEADS, width)
    bias = head_bias.reshape(KV_HEADS, GROUP).T.reshape(HEADS, 1)
    out = pl.pallas_call(
        stick_kernel,
        grid_spec=pltpu.PrefetchScalarGridSpec(
            num_scalar_prefetch=1,
            grid=(rows,),
            in_specs=[
                pl.BlockSpec((1, HEADS, width), lambda i, n: (i, 0, 0)),
                pl.BlockSpec((HEADS, 1), lambda i, n: (0, 0)),
                pl.BlockSpec((1, cache_len, width), lambda i, n: (i, 0, 0)),
                pl.BlockSpec((1, cache_len, width), lambda i, n: (i, 0, 0)),
            ],
            out_specs=pl.BlockSpec((1, GROUP, width), lambda i, n: (i, 0, 0)),
        ),
        out_shape=jax.ShapeDtypeStruct((rows, GROUP, width), F32),
        name="stick_attend",
    )(lengths, spread, bias, cache_key, cache_value)
    out = out.reshape(rows, GROUP, KV_HEADS, HEAD_DIM).transpose(0, 2, 1, 3)
    return out.reshape(rows, HEADS * HEAD_DIM).astype(BF16)


def local(
    chips,
    tokens,
    lengths,
    cache_key,
    cache_value,
    routes,
    route_logits,
    mix_gain,
    query_gain,
    key_gain,
    head_bias,
    w_query,
    w_key,
    w_value,
    w_out,
    ffn_gain,
    w_gate,
    w_up,
    w_down,
):
    rows, width = tokens.shape
    key_width = w_key.shape[1]
    query_width = w_query.shape[1]
    core = lax.rem(lax.axis_index(EP), 2)
    as_float = tokens.astype(F32)
    normed = rms_scaled(as_float, mix_gain).astype(BF16)
    x_blocks = normed.reshape(rows, chips, width // chips).transpose(1, 0, 2)
    wa = jnp.concatenate([w_query, w_key, w_value], axis=1)
    qkv, w_out_all = ring(x_blocks, wa, w_out.T, chips)
    queries = qkv[:, :query_width]
    fresh_key = qkv[:, query_width : query_width + key_width]
    fresh_value = qkv[:, query_width + key_width :]
    new_key = rms_scaled(fresh_key.reshape(rows, KV_HEADS, HEAD_DIM), key_gain)
    new_key = new_key.reshape(rows, key_width).astype(BF16)
    new_value = fresh_value.astype(BF16)
    attended = stick_attend(queries, lengths, cache_key, cache_value, query_gain, head_bias)
    w_out_all = w_out_all.reshape(width, w_out.shape[0])
    mixed = as_float + lax.dot_general(attended, w_out_all, (((1,), (1,)), ((), ())), preferred_element_type=F32)
    expert_in = rms_scaled(mixed, ffn_gain)

    gates = route_weights(routes, route_logits)
    coarse = lax.reduce_precision(gates, 8, 7)
    half = width // 2
    room = ((0, 0), (0, LANES - EXPERTS))
    x = jnp.concatenate([expert_in[:, :half], jnp.pad(coarse, room), expert_in[:, half:], jnp.pad(gates - coarse, room)], axis=1)
    every = all_rows(x, chips, 1)
    batch = chips * 2 * rows
    every = every.reshape(2, batch, half + LANES)
    ff_share = w_gate.shape[1]
    my_expert = lax.axis_index(EP) // (FF // ff_share)
    my_gate = lax.dynamic_slice_in_dim(every[:, :, half:].astype(F32).sum(0), my_expert, 1, 1)
    input_rows = jnp.concatenate([every[0, :, :half], every[1, :, :half]], axis=1)
    gate_value = jnp.dot(input_rows, w_gate, preferred_element_type=F32)
    up_value = jnp.dot(input_rows, w_up, preferred_element_type=F32)
    hidden = (jax.nn.silu(gate_value) * up_value * my_gate).astype(BF16)
    partial = jnp.dot(hidden, w_down, preferred_element_type=F32)
    sums = owner_sums(partial.reshape(NEAR, chips // NEAR, 2 * rows, width), chips, 2)
    sums = lax.dynamic_slice_in_dim(sums, core * rows, rows, 1)
    sums = sums.transpose(1, 0, 2).reshape(rows, width)
    return ((mixed + sums).astype(BF16), new_key, new_value)


def solution(mesh):
    chips = mesh.shape[EP] // 2
    both = ("grp", EP)
    in_specs = (
        P(both, None),
        P(both),
        P(both, None, None),
        P(both, None, None),
        P(both, None),
        P(both, None),
        P(),
        P(),
        P(),
        P(),
        P(EP, None),
        P(EP, None),
        P(EP, None),
        P(None, EP),
        P(),
        P(None, EP),
        P(None, EP),
        P(EP, None),
    )
    out_specs = (P(both, None), P(both, None), P(both, None))
    return jax.shard_map(functools.partial(local, chips), mesh=mesh, in_specs=in_specs, out_specs=out_specs, check_vma=False)
```
